512 devices in a mesh: rep: 2 (over z_hi), fs: 32 (over z_lo, y), tp: 8 (over x, core).
Axes of the slice: x: 4, y: 8, z: 8 (z_hi: 2, z_lo: 4; z = z_hi * 4 + z_lo), core: 2. Of those that a mesh axis runs over, the one named last changes fastest.
Arguments:
- later_input: bfloat16 [8192, 2048], P(('rep', 'fs')), may hold values from -6 to 6
- earlier_input: bfloat16 [8192, 2048], P(('rep', 'fs')), may hold values from -6 to 6
- cotangent: bfloat16 [8192, 2048], P(('rep', 'fs')), may hold values from -16 to 16
- gate_weight: bfloat16 [2048, 3072], P('fs', 'tp'), may hold values from -0.125 to 0.125
- up_weight: bfloat16 [2048, 3072], P('fs', 'tp'), may hold values from -0.125 to 0.125
- down_weight: bfloat16 [2048, 3072], P('fs', 'tp'), may hold values from -0.109375 to 0.109375
- gate_sum: float32 [2048, 3072], P('fs', 'tp'), may hold values from -192 to 192
- up_sum: float32 [2048, 3072], P('fs', 'tp'), may hold values from -192 to 192
- down_sum: float32 [2048, 3072], P('fs', 'tp'), may hold values from -192 to 192
Outputs:
- later_output: bfloat16 [8192, 2048], P(('rep', 'fs'))
- earlier_input_grad: bfloat16 [8192, 2048], P(('rep', 'fs'))
- gate_sum_new: float32 [2048, 3072], P('fs', 'tp')
- up_sum_new: float32 [2048, 3072], P('fs', 'tp')
- down_sum_new: float32 [2048, 3072], P('fs', 'tp')
The draws below stay inside these ranges and needn't reach their ends.
All inputs are finite; a program needn't handle non-finite values.
Results may differ from the reference program's by a relative error of at most 0.02.
Values may be sent and summed in bfloat16 or wider, within the bound.
No kernel may reach another device: no remote copies, remote signals or barrier semaphores. Data moves between devices by JAX's collectives and lax.ppermute only.
A program may use at most 128 MiB of HBM per device.

```python
import jax
import jax.numpy as jnp
from jax import lax

D = 2048
FF = 3072
TOKENS = 8192
N_TP = 8


def with_spikes(values, rng, source, target, blocks, factor):
    owner, partner = [(jnp.arange(values.shape[dim]) // (values.shape[dim] // blocks)).reshape([-1 if axis == dim else 1 for axis in range(values.ndim)]) for dim in (source, target)]
    chosen = jax.random.permutation(rng, blocks)[partner]
    strong = (owner == chosen) | (owner == (partner + blocks // 2) % blocks)
    return jnp.where(strong, factor * values, values)


def block_scale(key, extent, shards, smallest, largest):
    factor_of = 1.0
    for dim, parts in shards:
        heights = jax.random.uniform(jax.random.fold_in(jax.random.fold_in(key, 6), dim), (parts,), jnp.float32, smallest / len(shards), largest / len(shards))
        factor_of = factor_of * jnp.repeat(jnp.exp(heights), extent[dim] // parts).reshape((-1,) + (1,) * (len(extent) - 1 - dim))
    return factor_of


def normal_values(own_key, extent, scale, limit, pieces=(), kind=jnp.bfloat16):
    entries = scale * jax.random.normal(own_key, extent, jnp.float32)
    if pieces:
        entries = entries * block_scale(own_key, extent, pieces, -0.22, 0.18)
    return jnp.clip(entries, -limit, limit).astype(kind)


def bell_draw_with(rng, dims, scale, reach, split, heavy, held_as=jnp.bfloat16):
    values = scale * jax.random.normal(rng, dims, jnp.float32)
    if split:
        values = values * block_scale(rng, dims, split, -0.22, 0.18)
    return jnp.clip(with_spikes(values, jax.random.fold_in(rng, 3), *heavy), -reach, reach).astype(held_as)


def setup_inputs(seed: int = 0) -> dict:
    arg_keys = jax.random.split(jax.random.key(seed), 10)
    return {
        "later_input": normal_values(arg_keys[0], (TOKENS, D), 1.0, 6.0, ((0, 64),)),
        "earlier_input": normal_values(arg_keys[1], (TOKENS, D), 1.0, 6.0, ((0, 64),)),
        "cotangent": bell_draw_with(arg_keys[2], (TOKENS, D), 1.0, 16.0, ((0, 64),), (0, 1, 64, 4.0)),
        "gate_weight": normal_values(arg_keys[3], (D, FF), D ** -0.5, 0.125, ((0, 32), (1, 8))),
        "up_weight": normal_values(arg_keys[4], (D, FF), D ** -0.5, 0.125, ((0, 32), (1, 8))),
        "down_weight": normal_values(arg_keys[5], (D, FF), FF ** -0.5, 0.109375, ((0, 32), (1, 8))),
        "gate_sum": normal_values(arg_keys[6], (D, FF), 32.0, 192.0, ((0, 32), (1, 8)), jnp.float32),
        "up_sum": normal_values(arg_keys[7], (D, FF), 32.0, 192.0, ((0, 32), (1, 8)), jnp.float32),
        "down_sum": normal_values(arg_keys[8], (D, FF), 32.0, 192.0, ((0, 32), (1, 8)), jnp.float32),
    }


def contract_last(first, second):
    return lax.dot_general(first, second, (((1,), (1,)), ((), ())), preferred_element_type=jnp.float32)


def contract_first(first, second):
    return lax.dot_general(first, second, (((0,), (0,)), ((), ())), preferred_element_type=jnp.float32)


def blockwise(firsts, seconds):
    block_width = FF // N_TP
    running = jnp.zeros((firsts[0].shape[0], seconds[0].shape[0]), jnp.float32)
    for block_index in range(N_TP):
        lower = block_index * block_width
        partial_value = jnp.zeros_like(running)
        for first, second in zip(firsts, seconds):
            partial_value = partial_value + contract_last(first[:, lower:lower + block_width], second[:, lower:lower + block_width])
        rounded = lax.optimization_barrier(partial_value.astype(jnp.bfloat16))
        running = running + rounded.astype(jnp.float32)
    return running.astype(jnp.bfloat16)


def reference(later_input, earlier_input, cotangent, gate_weight, up_weight, down_weight, gate_sum, up_sum, down_sum):
    gate_late = jnp.dot(later_input, gate_weight, preferred_element_type=jnp.float32)
    up_late = jnp.dot(later_input, up_weight, preferred_element_type=jnp.float32)
    hidden_late = (jax.nn.silu(gate_late) * up_late).astype(jnp.bfloat16)
    later_output = blockwise([hidden_late], [down_weight])
    gate_early = jnp.dot(earlier_input, gate_weight, preferred_element_type=jnp.float32)
    up_early = jnp.dot(earlier_input, up_weight, preferred_element_type=jnp.float32)
    hidden_grad = jnp.dot(cotangent, down_weight, preferred_element_type=jnp.float32)
    sigmoid_gate = jax.nn.sigmoid(gate_early)
    silu_early = gate_early * sigmoid_gate
    gate_grad = (hidden_grad * up_early * sigmoid_gate * (1.0 + gate_early * (1.0 - sigmoid_gate))).astype(jnp.bfloat16)
    up_grad = (hidden_grad * silu_early).astype(jnp.bfloat16)
    hidden_early = (silu_early * up_early).astype(jnp.bfloat16)
    earlier_input_grad = blockwise([gate_grad, up_grad], [gate_weight, up_weight])
    gate_sum_new = gate_sum + contract_first(earlier_input, gate_grad)
    up_sum_new = up_sum + contract_first(earlier_input, up_grad)
    down_sum_new = down_sum + contract_first(cotangent, hidden_early)
    return later_output, earlier_input_grad, gate_sum_new, up_sum_new, down_sum_new
```

```python
import jax
import jax.numpy as jnp
from jax import lax
from jax.sharding import Mesh, PartitionSpec as P


NZ = 8
NZL = 4
NY = 8
RING = ("zh", "zl")
TP = ("x", "c")
SHIFTS = (1, -1, -2)


def shift_z(array, by):
    return lax.ppermute(array, RING, [(i, (i + by) % NZ) for i in range(NZ)])


def contract_last(first, second):
    return lax.dot_general(
        first, second, (((1,), (1,)), ((), ())), preferred_element_type=jnp.float32
    )


def contract_first(first, second):
    return lax.dot_general(
        first, second, (((0,), (0,)), ((), ())), preferred_element_type=jnp.float32
    )


def dot(first, second):
    return jnp.dot(first, second, preferred_element_type=jnp.float32)


def halves_first(array, count):
    rows, columns = array.shape
    parts = array.reshape(rows, count, 2, columns // (2 * count))
    return parts.transpose(0, 2, 1, 3).reshape(rows, columns)


def halves_back(array, count):
    rows, columns = array.shape
    parts = array.reshape(rows, 2, count, columns // (2 * count))
    return parts.transpose(0, 2, 1, 3).reshape(rows, columns)


def sum_over_tp(partial):
    n = lax.axis_size(TP)
    rows, columns = partial.shape
    blocks = partial.reshape(n, rows // n, columns)
    blocks = lax.all_to_all(blocks, TP, split_axis=0, concat_axis=0, tiled=True)
    own = jnp.sum(blocks.astype(jnp.float32), axis=0).astype(jnp.bfloat16)
    copies = jnp.broadcast_to(own, (n, *own.shape))
    out = lax.all_to_all(copies, TP, split_axis=0, concat_axis=0, tiled=True)
    return out.reshape(rows, columns)


def per_device(
    later_input,
    earlier_input,
    cotangent,
    gate_weight,
    up_weight,
    down_weight,
    gate_sum,
    up_sum,
    down_sum,
):
    bf = jnp.bfloat16
    n_fs = NZL * NY
    zh = lax.axis_index("zh")
    zl = lax.axis_index("zl")
    rows, width = gate_weight.shape
    shards = jnp.concatenate((gate_weight, up_weight, down_weight), axis=1)
    half = lax.dynamic_slice_in_dim(shards, zh * (rows // 2), rows // 2, 0)
    full = lax.all_gather(half, ("zh", "zl", "y"), axis=0, tiled=True)
    gate_full, up_full, down_full = (
        full[:, :width],
        full[:, width : 2 * width],
        full[:, 2 * width :],
    )

    block = rows * NY

    def features_for(where):
        cut = lambda a: lax.dynamic_slice_in_dim(a, where * block, block, 1)
        return jnp.concatenate((cut(earlier_input), cut(cotangent)), axis=1)

    features = [features_for(zl)] + [
        shift_z(features_for(jnp.mod(zl + by + NZL, NZL)), by) for by in SHIFTS
    ]

    early = halves_first(earlier_input, n_fs)
    cot = halves_first(cotangent, n_fs)
    late = halves_first(later_input, n_fs)

    gate_early = dot(early, gate_full)
    up_early = dot(early, up_full)
    hidden_grad = dot(cot, down_full)
    sigmoid_gate = jax.nn.sigmoid(gate_early)
    silu_early = gate_early * sigmoid_gate
    gate_grad = (
        hidden_grad * up_early * sigmoid_gate * (1.0 + gate_early * (1.0 - sigmoid_gate))
    ).astype(bf)
    up_grad = (hidden_grad * silu_early).astype(bf)
    hidden_early = (silu_early * up_early).astype(bf)

    piece = jnp.concatenate((gate_grad, up_grad, hidden_early), axis=1)
    pieces = [piece] + [shift_z(piece, by) for by in SHIFTS]

    gate_late = dot(late, gate_full)
    up_late = dot(late, up_full)
    hidden_late = (jax.nn.silu(gate_late) * up_late).astype(bf)
    partial_late = contract_last(hidden_late, down_full).astype(bf)
    partial_early = (
        contract_last(gate_grad, gate_full) + contract_last(up_grad, up_full)
    ).astype(bf)
    tokens = partial_late.shape[0]
    n_tp = lax.axis_size(TP)
    both = jnp.concatenate(
        (
            partial_late.reshape(n_tp, tokens // n_tp, -1),
            partial_early.reshape(n_tp, tokens // n_tp, -1),
        ),
        axis=1,
    )
    both = lax.all_to_all(both, TP, split_axis=0, concat_axis=0, tiled=True)
    own = jnp.sum(both.astype(jnp.float32), axis=0).astype(bf)
    own = halves_back(own, n_fs)
    copies = jnp.broadcast_to(own, (n_tp, *own.shape))
    outs = lax.all_to_all(copies, TP, split_axis=0, concat_axis=0, tiled=True)
    later_output = outs[:, : tokens // n_tp].reshape(tokens, -1)
    earlier_input_grad = outs[:, tokens // n_tp :].reshape(tokens, -1)

    first = jnp.concatenate(features, axis=0)
    second = jnp.concatenate(pieces, axis=0)
    both_local = contract_first(first[:, :block], second[:, : 2 * width])
    down_local = contract_first(first[:, block:], second[:, 2 * width :])
    local = jnp.concatenate((both_local.astype(bf), down_local.astype(bf)), axis=1)
    local = local.reshape(NY, rows, 3 * width)
    local = lax.all_to_all(local, "y", split_axis=0, concat_axis=0, tiled=True)
    mine = jnp.sum(local.astype(jnp.float32), axis=0).astype(bf)
    other = lax.ppermute(mine, "zh", [(0, 1), (1, 0)])
    total = mine.astype(jnp.float32) + other.astype(jnp.float32)
    return (
        later_output,
        earlier_input_grad,
        gate_sum + total[:, :width],
        up_sum + total[:, width : 2 * width],
        down_sum + total[:, 2 * width :],
    )


def solution(mesh):
    fine = Mesh(mesh.devices.reshape(2, NZL, NY, -1, 2), ("zh", "zl", "y", "x", "c"))
    tokens = P(("zh", "zl", "y"), None)
    weights = P(("zl", "y"), ("x", "c"))
    return jax.shard_map(
        per_device,
        mesh=fine,
        in_specs=(tokens,) * 3 + (weights,) * 6,
        out_specs=(tokens,) * 2 + (weights,) * 3,
        check_vma=False,
    )
```

```python
import jax
import jax.numpy as jnp
from jax import lax
from jax.sharding import Mesh, PartitionSpec as P


NZ = 8
NZL = 4
NY = 8
RING = ("zh", "zl")
TP = ("x", "c")
SHIFTS = (1, -1, -2)


def shift_z(array, by):
    return lax.ppermute(array, RING, [(i, (i + by) % NZ) for i in range(NZ)])


def contract_last(first, second):
    return lax.dot_general(
        first, second, (((1,), (1,)), ((), ())), preferred_element_type=jnp.float32
    )


def contract_first(first, second):
    return lax.dot_general(
        first, second, (((0,), (0,)), ((), ())), preferred_element_type=jnp.float32
    )


def dot(first, second):
    return jnp.dot(first, second, preferred_element_type=jnp.float32)


def shift(array, axis, count, by):
    return lax.ppermute(array, axis, [(i, (i + by) % count) for i in range(count)])


def put(buffer, block, at, dim=0):
    return lax.dynamic_update_slice_in_dim(buffer, jnp.expand_dims(block, dim), at, dim)


def swap_columns(array, outer, inner):
    rows, columns = array.shape
    parts = array.reshape(rows, outer, inner, columns // (outer * inner))
    return parts.transpose(0, 2, 1, 3).reshape(rows, columns)


def gather_z_then_y(shard, zl, y):
    near = jnp.zeros((NZL, *shard.shape), shard.dtype)
    near = put(near, shard, zl)
    for by in SHIFTS:
        near = put(near, shift_z(shard, by), jnp.mod(zl - by + NZL, NZL))
    full = jnp.zeros((NY, *near.shape), shard.dtype)
    full = put(full, near, y)
    up = down = near
    for step in range(1, NY // 2 + 1):
        up = shift(up, "y", NY, 1)
        full = put(full, up, jnp.mod(y - step + NY, NY))
        if step < NY // 2:
            down = shift(down, "y", NY, -1)
            full = put(full, down, jnp.mod(y + step, NY))
    return full


def gather_y_then_z(shard, zl):
    copies = jnp.broadcast_to(shard, (NY, *shard.shape))
    column = lax.all_to_all(copies, "y", split_axis=0, concat_axis=0, tiled=True)
    full = jnp.zeros((NY, NZL, *shard.shape), shard.dtype)
    full = put(full, column, zl, 1)
    for by in (1, -1):
        full = put(full, shift_z(column, by), jnp.mod(zl - by + NZL, NZL), 1)
    far = jnp.concatenate(
        (shift_z(column[: NY // 2], 2), shift_z(column[NY // 2 :], -2)), axis=0
    )
    return put(full, far, jnp.mod(zl + 2, NZL), 1)


def everywhere_on_tp(own, x, c):
    n_x = lax.axis_size("x")
    line = jnp.zeros((n_x, *own.shape), own.dtype)
    line = put(line, own, x)
    for by in (1, -1, 2):
        line = put(line, shift(own, "x", n_x, by), jnp.mod(x - by + n_x, n_x))
    other = lax.ppermute(line, "c", [(0, 1), (1, 0)])
    both = jnp.zeros((n_x, 2, *own.shape), own.dtype)
    both = put(both, line, c, 1)
    both = put(both, other, 1 - c, 1)
    return both.reshape(2 * n_x, *own.shape)


def per_device(
    later_input,
    earlier_input,
    cotangent,
    gate_weight,
    up_weight,
    down_weight,
    gate_sum,
    up_sum,
    down_sum,
):
    bf = jnp.bfloat16
    zl = lax.axis_index("zl")
    y = lax.axis_index("y")
    rows, width = gate_weight.shape
    shards = jnp.concatenate((gate_weight, up_weight, down_weight), axis=1)
    cut = 640
    part_a = gather_z_then_y(shards[:, :cut], zl, y).reshape(-1, cut)
    part_b = gather_y_then_z(shards[:, cut:], zl).reshape(-1, 3 * width - cut)
    gate_full = part_a[:, :width]
    up_a = part_a[:, width:]
    up_b = part_b[:, : 2 * width - cut]
    down_full = part_b[:, 2 * width - cut :]
    n_a = up_a.shape[1]

    def up_dot(array):
        return jnp.concatenate((dot(array, up_a), dot(array, up_b)), axis=1)

    block = rows * NY

    def features_for(where):
        cut = lambda a: lax.dynamic_slice_in_dim(a, where * block, block, 1)
        return jnp.concatenate((cut(earlier_input), cut(cotangent)), axis=1)

    features = [features_for(zl)] + [
        shift_z(features_for(jnp.mod(zl + by + NZL, NZL)), by) for by in SHIFTS
    ]

    early = swap_columns(earlier_input, NZL, NY)
    cot = swap_columns(cotangent, NZL, NY)
    late = swap_columns(later_input, NZL, NY)

    gate_early = dot(early, gate_full)
    up_early = up_dot(early)
    hidden_grad = dot(cot, down_full)
    sigmoid_gate = jax.nn.sigmoid(gate_early)
    silu_early = gate_early * sigmoid_gate
    gate_grad = (
        hidden_grad * up_early * sigmoid_gate * (1.0 + gate_early * (1.0 - sigmoid_gate))
    ).astype(bf)
    up_grad = (hidden_grad * silu_early).astype(bf)
    hidden_early = (silu_early * up_early).astype(bf)

    piece = jnp.concatenate((gate_grad, up_grad, hidden_early), axis=1)
    pieces = [piece] + [shift_z(piece, by) for by in SHIFTS]

    gate_late = dot(late, gate_full)
    up_late = up_dot(late)
    hidden_late = (jax.nn.silu(gate_late) * up_late).astype(bf)
    partial_late = contract_last(hidden_late, down_full).astype(bf)
    partial_early = (
        contract_last(gate_grad, gate_full)
        + contract_last(up_grad[:, :n_a], up_a)
        + contract_last(up_grad[:, n_a:], up_b)
    ).astype(bf)
    tokens = partial_late.shape[0]
    n_tp = lax.axis_size(TP)
    both = jnp.concatenate(
        (
            partial_late.reshape(n_tp, tokens // n_tp, -1),
            partial_early.reshape(n_tp, tokens // n_tp, -1),
        ),
        axis=1,
    )
    both = lax.all_to_all(both, TP, split_axis=0, concat_axis=0, tiled=True)
    own = jnp.sum(both.astype(jnp.float32), axis=0).astype(bf)
    own = swap_columns(own, NY, NZL)
    outs = everywhere_on_tp(own, lax.axis_index("x"), lax.axis_index("c"))
    later_output = outs[:, : tokens // n_tp].reshape(tokens, -1)
    earlier_input_grad = outs[:, tokens // n_tp :].reshape(tokens, -1)

    first = jnp.concatenate(features, axis=0)
    second = jnp.concatenate(pieces, axis=0)
    both_local = contract_first(first[:, :block], second[:, : 2 * width])
    down_local = contract_first(first[:, block:], second[:, 2 * width :])
    local = jnp.concatenate((both_local.astype(bf), down_local.astype(bf)), axis=1)
    local = local.reshape(NY, rows, 3 * width)
    local = lax.all_to_all(local, "y", split_axis=0, concat_axis=0, tiled=True)
    mine = jnp.sum(local.astype(jnp.float32), axis=0).astype(bf)
    other = lax.ppermute(mine, "zh", [(0, 1), (1, 0)])
    total = mine.astype(jnp.float32) + other.astype(jnp.float32)
    return (
        later_output,
        earlier_input_grad,
        gate_sum + total[:, :width],
        up_sum + total[:, width : 2 * width],
        down_sum + total[:, 2 * width :],
    )


def solution(mesh):
    fine = Mesh(mesh.devices.reshape(2, NZL, NY, -1, 2), ("zh", "zl", "y", "x", "c"))
    tokens = P(("zh", "zl", "y"), None)
    weights = P(("zl", "y"), ("x", "c"))
    return jax.shard_map(
        per_device,
        mesh=fine,
        in_specs=(tokens,) * 3 + (weights,) * 6,
        out_specs=(tokens,) * 2 + (weights,) * 3,
        check_vma=False,
    )
```

```python
import jax
import jax.numpy as jnp
from jax import lax
from jax.sharding import Mesh, PartitionSpec as P


NZ = 8
NZL = 4
NY = 8
RING = ("zh", "zl")
TP = ("x", "c")
SHIFTS = (1, -1, -2)


def shift_z(array, by):
    return lax.ppermute(array, RING, [(i, (i + by) % NZ) for i in range(NZ)])


def contract_last(first, second):
    return lax.dot_general(
        first, second, (((1,), (1,)), ((), ())), preferred_element_type=jnp.float32
    )


def contract_first(first, second):
    return lax.dot_general(
        first, second, (((0,), (0,)), ((), ())), preferred_element_type=jnp.float32
    )


def dot(first, second):
    return jnp.dot(first, second, preferred_element_type=jnp.float32)


def shift(array, axis, count, by):
    return lax.ppermute(array, axis, [(i, (i + by) % count) for i in range(count)])


def put(buffer, block, at, dim=0):
    return lax.dynamic_update_slice_in_dim(buffer, jnp.expand_dims(block, dim), at, dim)


def swap_columns(array, outer, inner):
    rows, columns = array.shape
    parts = array.reshape(rows, outer, inner, columns // (outer * inner))
    return parts.transpose(0, 2, 1, 3).reshape(rows, columns)


def spread_y(block):
    copies = jnp.broadcast_to(block, (NY, *block.shape))
    return lax.all_to_all(copies, "y", split_axis=0, concat_axis=0, tiled=True)


def gather_z_then_y(shard, zl):
    near = jnp.zeros((NZL, *shard.shape), shard.dtype)
    near = put(near, shard, zl)
    for by in SHIFTS:
        near = put(near, shift_z(shard, by), jnp.mod(zl - by + NZL, NZL))
    return spread_y(near)


def gather_y_then_z(shard, zl):
    column = spread_y(shard)
    full = jnp.zeros((NY, NZL, *shard.shape), shard.dtype)
    full = put(full, column, zl, 1)
    for by in (1, -1):
        full = put(full, shift_z(column, by), jnp.mod(zl - by + NZL, NZL), 1)
    far = jnp.concatenate(
        (shift_z(column[: NY // 2], 2), shift_z(column[NY // 2 :], -2)), axis=0
    )
    return put(full, far, jnp.mod(zl + 2, NZL), 1)


def reduce_on_tp(late, early, x, c):
    n_x = lax.axis_size("x")
    tokens, width = late.shape
    cut = lambda a: a.reshape(n_x, 2, tokens // (2 * n_x), width)
    both = jnp.concatenate((cut(late), cut(early)), axis=2)
    pick = lambda at: lax.dynamic_index_in_dim(both, at, 1, keepdims=False)
    other = lax.ppermute(pick(1 - c), "c", [(0, 1), (1, 0)])
    pair = (pick(c).astype(jnp.float32) + other.astype(jnp.float32)).astype(late.dtype)
    part = lambda at: lax.dynamic_index_in_dim(pair, at, 0, keepdims=False)
    total = part(x).astype(jnp.float32)
    for by in (1, -1, 2):
        sent = shift(part(jnp.mod(x + by + n_x, n_x)), "x", n_x, by)
        total = total + sent.astype(jnp.float32)
    return total.astype(late.dtype)


def everywhere_on_tp(own, x, c):
    n_x = lax.axis_size("x")
    line = jnp.zeros((n_x, *own.shape), own.dtype)
    line = put(line, own, x)
    for by in (1, -1, 2):
        line = put(line, shift(own, "x", n_x, by), jnp.mod(x - by + n_x, n_x))
    other = lax.ppermute(line, "c", [(0, 1), (1, 0)])
    both = jnp.zeros((n_x, 2, *own.shape), own.dtype)
    both = put(both, line, c, 1)
    both = put(both, other, 1 - c, 1)
    return both.reshape(2 * n_x, *own.shape)


def per_device(
    later_input,
    earlier_input,
    cotangent,
    gate_weight,
    up_weight,
    down_weight,
    gate_sum,
    up_sum,
    down_sum,
):
    bf = jnp.bfloat16
    zl = lax.axis_index("zl")
    y = lax.axis_index("y")
    rows, width = gate_weight.shape
    later_half = jnp.concatenate((up_weight, down_weight), axis=1)
    part_b = gather_y_then_z(later_half, zl).reshape(-1, 2 * width)
    gate_full = gather_z_then_y(gate_weight, zl).reshape(-1, width)
    up_full = part_b[:, :width]
    down_full = part_b[:, width:]

    block = rows * NY

    def features_for(where):
        cut = lambda a: lax.dynamic_slice_in_dim(a, where * block, block, 1)
        return jnp.concatenate((cut(earlier_input), cut(cotangent)), axis=1)

    features = [features_for(zl)] + [
        shift_z(features_for(jnp.mod(zl + by + NZL, NZL)), by) for by in SHIFTS
    ]

    early = swap_columns(earlier_input, NZL, NY)
    cot = swap_columns(cotangent, NZL, NY)
    late = swap_columns(later_input, NZL, NY)

    gate_early = dot(early, gate_full)
    up_early = dot(early, up_full)
    hidden_grad = dot(cot, down_full)
    sigmoid_gate = jax.nn.sigmoid(gate_early)
    silu_early = gate_early * sigmoid_gate
    gate_grad = (
        hidden_grad * up_early * sigmoid_gate * (1.0 + gate_early * (1.0 - sigmoid_gate))
    ).astype(bf)
    up_grad = (hidden_grad * silu_early).astype(bf)
    hidden_early = (silu_early * up_early).astype(bf)

    piece = jnp.concatenate((gate_grad, up_grad, hidden_early), axis=1)
    pieces = [piece] + [shift_z(piece, by) for by in SHIFTS]

    gate_late = dot(late, gate_full)
    up_late = dot(late, up_full)
    hidden_late = (jax.nn.silu(gate_late) * up_late).astype(bf)
    partial_late = contract_last(hidden_late, down_full).astype(bf)
    partial_early = (
        contract_last(gate_grad, gate_full)
        + contract_last(up_grad, up_full)
    ).astype(bf)
    tokens = partial_late.shape[0]
    n_tp = lax.axis_size(TP)
    x, c = lax.axis_index("x"), lax.axis_index("c")
    own = reduce_on_tp(partial_late, partial_early, x, c)
    own = swap_columns(own, NY, NZL)
    outs = everywhere_on_tp(own, x, c)
    later_output = outs[:, : tokens // n_tp].reshape(tokens, -1)
    earlier_input_grad = outs[:, tokens // n_tp :].reshape(tokens, -1)

    first = jnp.concatenate(features, axis=0)
    second = jnp.concatenate(pieces, axis=0)
    both_local = contract_first(first[:, :block], second[:, : 2 * width])
    down_local = contract_first(first[:, block:], second[:, 2 * width :])
    local = jnp.concatenate((both_local.astype(bf), down_local.astype(bf)), axis=1)
    local = local.reshape(NY, rows, 3 * width)
    local = lax.all_to_all(local, "y", split_axis=0, concat_axis=0, tiled=True)
    mine = jnp.sum(local.astype(jnp.float32), axis=0).astype(bf)
    other = lax.ppermute(mine, "zh", [(0, 1), (1, 0)])
    total = mine.astype(jnp.float32) + other.astype(jnp.float32)
    return (
        later_output,
        earlier_input_grad,
        gate_sum + total[:, :width],
        up_sum + total[:, width : 2 * width],
        down_sum + total[:, 2 * width :],
    )


def solution(mesh):
    fine = Mesh(mesh.devices.reshape(2, NZL, NY, -1, 2), ("zh", "zl", "y", "x", "c"))
    tokens = P(("zh", "zl", "y"), None)
    weights = P(("zl", "y"), ("x", "c"))
    return jax.shard_map(
        per_device,
        mesh=fine,
        in_specs=(tokens,) * 3 + (weights,) * 6,
        out_specs=(tokens,) * 2 + (weights,) * 3,
        check_vma=False,
    )
```

```python
import jax
import jax.numpy as jnp
from jax import lax
from jax.sharding import Mesh, PartitionSpec as P


NZ = 8
NZL = 4
NY = 8
RING = ("zh", "zl")
TP = ("x", "c")
SHIFTS = (1, -1, -2)


def shift_z(array, by):
    return lax.ppermute(array, RING, [(i, (i + by) % NZ) for i in range(NZ)])


def contract_last(first, second):
    return lax.dot_general(
        first, second, (((1,), (1,)), ((), ())), preferred_element_type=jnp.float32
    )


def contract_first(first, second):
    return lax.dot_general(
        first, second, (((0,), (0,)), ((), ())), preferred_element_type=jnp.float32
    )


def dot(first, second):
    return jnp.dot(first, second, preferred_element_type=jnp.float32)


def shift(array, axis, count, by):
    return lax.ppermute(array, axis, [(i, (i + by) % count) for i in range(count)])


def put(buffer, block, at, dim=0):
    return lax.dynamic_update_slice_in_dim(buffer, jnp.expand_dims(block, dim), at, dim)


def swap_columns(array, outer, inner):
    rows, columns = array.shape
    parts = array.reshape(rows, outer, inner, columns // (outer * inner))
    return parts.transpose(0, 2, 1, 3).reshape(rows, columns)


def spread_y(block):
    copies = jnp.broadcast_to(block, (NY, *block.shape))
    return lax.all_to_all(copies, "y", split_axis=0, concat_axis=0, tiled=True)


def gather_z_then_y(shard, zl):
    near = jnp.zeros((NZL, *shard.shape), shard.dtype)
    near = put(near, shard, zl)
    for by in SHIFTS:
        block = shift_z(shard, by)
        near = put(near, block, jnp.mod(zl - by + NZL, NZL))
    return spread_y(near)


def gather_y_then_z(shard, zl):
    column = spread_y(shard)
    full = jnp.zeros((NY, NZL, *shard.shape), shard.dtype)
    full = put(full, column, zl, 1)
    for by in (1, -1):
        block = shift_z(column, by)
        full = put(full, block, jnp.mod(zl - by + NZL, NZL), 1)
    far_low = shift_z(column[: NY // 2], 2)
    far_high = shift_z(column[NY // 2 :], -2)
    far = jnp.concatenate((far_low, far_high), axis=0)
    return put(full, far, jnp.mod(zl + 2, NZL), 1)


def reduce_on_tp(late, early, x, c):
    n_x = lax.axis_size("x")
    tokens, width = late.shape
    cut = lambda a: a.reshape(n_x, 2, tokens // (2 * n_x), width)
    both = jnp.concatenate((cut(late), cut(early)), axis=2)
    pick = lambda at: lax.dynamic_index_in_dim(both, at, 1, keepdims=False)
    other = lax.ppermute(pick(1 - c), "c", [(0, 1), (1, 0)])
    pair = (pick(c).astype(jnp.float32) + other.astype(jnp.float32)).astype(late.dtype)
    part = lambda at: lax.dynamic_index_in_dim(pair, at, 0, keepdims=False)
    total = part(x).astype(jnp.float32)
    for by in (1, -1, 2):
        block = part(jnp.mod(x + by + n_x, n_x))
        sent = shift(block, "x", n_x, by)
        total = total + sent.astype(jnp.float32)
    return total.astype(late.dtype)


def everywhere_on_tp(own, x, c):
    n_x = lax.axis_size("x")
    line = jnp.zeros((n_x, *own.shape), own.dtype)
    line = put(line, own, x)
    for by in (1, -1, 2):
        line = put(line, shift(own, "x", n_x, by), jnp.mod(x - by + n_x, n_x))
    other = lax.ppermute(line, "c", [(0, 1), (1, 0)])
    both = jnp.zeros((n_x, 2, *own.shape), own.dtype)
    both = put(both, line, c, 1)
    both = put(both, other, 1 - c, 1)
    return both.reshape(2 * n_x, *own.shape)


def per_device(
    later_input,
    earlier_input,
    cotangent,
    gate_weight,
    up_weight,
    down_weight,
    gate_sum,
    up_sum,
    down_sum,
):
    bf = jnp.bfloat16
    zl = lax.axis_index("zl")
    rows, width = gate_weight.shape
    later_half = jnp.concatenate((up_weight, down_weight), axis=1)
    part_b = gather_y_then_z(later_half, zl).reshape(-1, 2 * width)
    gate_full = gather_z_then_y(gate_weight, zl).reshape(-1, width)
    up_full = part_b[:, :width]
    down_full = part_b[:, width:]

    block = rows * NY

    def features_for(where):
        cut = lambda a: lax.dynamic_slice_in_dim(a, where * block, block, 1)
        return jnp.concatenate((cut(earlier_input), cut(cotangent)), axis=1)

    features = [features_for(zl)]
    for by in SHIFTS:
        sent = features_for(jnp.mod(zl + by + NZL, NZL))
        features.append(shift_z(sent, by))

    early = swap_columns(earlier_input, NZL, NY)
    cot = swap_columns(cotangent, NZL, NY)
    late = swap_columns(later_input, NZL, NY)

    gate_early = dot(early, gate_full)
    up_early = dot(early, up_full)
    hidden_grad = dot(cot, down_full)
    sigmoid_gate = jax.nn.sigmoid(gate_early)
    silu_early = gate_early * sigmoid_gate
    gate_grad = (
        hidden_grad * up_early * sigmoid_gate * (1.0 + gate_early * (1.0 - sigmoid_gate))
    ).astype(bf)
    up_grad = (hidden_grad * silu_early).astype(bf)
    hidden_early = (silu_early * up_early).astype(bf)

    piece = jnp.concatenate((gate_grad, up_grad, hidden_early), axis=1)
    pieces = [piece] + [shift_z(piece, by) for by in SHIFTS]

    gate_late = dot(late, gate_full)
    up_late = dot(late, up_full)
    hidden_late = (jax.nn.silu(gate_late) * up_late).astype(bf)
    partial_late = contract_last(hidden_late, down_full).astype(bf)
    partial_early = (
        contract_last(gate_grad, gate_full) + contract_last(up_grad, up_full)
    ).astype(bf)
    tokens = partial_late.shape[0]
    n_tp = lax.axis_size(TP)
    x, c = lax.axis_index("x"), lax.axis_index("c")
    own = reduce_on_tp(partial_late, partial_early, x, c)
    own = swap_columns(own, NY, NZL)
    outs = everywhere_on_tp(own, x, c)
    later_output = outs[:, : tokens // n_tp].reshape(tokens, -1)
    earlier_input_grad = outs[:, tokens // n_tp :].reshape(tokens, -1)

    first = jnp.concatenate(features, axis=0)
    second = jnp.concatenate(pieces, axis=0)
    both_local = contract_first(first[:, :block], second[:, : 2 * width])
    down_local = contract_first(first[:, block:], second[:, 2 * width :])
    local = jnp.concatenate((both_local.astype(bf), down_local.astype(bf)), axis=1)
    local = local.reshape(NY, rows, 3 * width)
    local = lax.all_to_all(local, "y", split_axis=0, concat_axis=0, tiled=True)
    mine = jnp.sum(local.astype(jnp.float32), axis=0).astype(bf)
    other = lax.ppermute(mine, "zh", [(0, 1), (1, 0)])
    total = mine.astype(jnp.float32) + other.astype(jnp.float32)
    return (
        later_output,
        earlier_input_grad,
        gate_sum + total[:, :width],
        up_sum + total[:, width : 2 * width],
        down_sum + total[:, 2 * width :],
    )


def solution(mesh):
    fine = Mesh(mesh.devices.reshape(2, NZL, NY, -1, 2), ("zh", "zl", "y", "x", "c"))
    tokens = P(("zh", "zl", "y"), None)
    weights = P(("zl", "y"), ("x", "c"))
    return jax.shard_map(
        per_device,
        mesh=fine,
        in_specs=(tokens,) * 3 + (weights,) * 6,
        out_specs=(tokens,) * 2 + (weights,) * 3,
        check_vma=False,
    )
```

```python
import jax
import jax.numpy as jnp
from jax import lax
from jax.sharding import Mesh, PartitionSpec as P


NZ = 8
NZL = 4
NY = 8
RING = ("zh", "zl")
TP = ("x", "c")
SHIFTS = (1, -1, -2)


def shift_z(array, by):
    return lax.ppermute(array, RING, [(i, (i + by) % NZ) for i in range(NZ)])


def contract_last(first, second):
    return lax.dot_general(
        first, second, (((1,), (1,)), ((), ())), preferred_element_type=jnp.float32
    )


def contract_first(first, second):
    return lax.dot_general(
        first, second, (((0,), (0,)), ((), ())), preferred_element_type=jnp.float32
    )


def dot(first, second):
    return jnp.dot(first, second, preferred_element_type=jnp.float32)


def shift(array, axis, count, by):
    return lax.ppermute(array, axis, [(i, (i + by) % count) for i in range(count)])


def put(buffer, block, at, dim=0):
    return lax.dynamic_update_slice_in_dim(buffer, jnp.expand_dims(block, dim), at, dim)


def spread_y(block):
    return lax.all_to_all(block, "y", split_axis=0, concat_axis=0, tiled=True)


def gather_z_then_y(shard, zl):
    near = jnp.zeros((NZL, *shard.shape), shard.dtype)
    near = put(near, shard, zl)
    for by in SHIFTS:
        block = shift_z(shard, by)
        near = put(near, block, jnp.mod(zl - by + NZL, NZL))
    full = spread_y(jnp.broadcast_to(near, (NY, *near.shape)))
    return full.transpose(1, 0, 2, 3)


def gather_y_then_z(shards, zl):
    shard = jnp.concatenate(shards, axis=1)
    column = spread_y(jnp.broadcast_to(shard, (NY, *shard.shape)))
    full = jnp.zeros((NZL, *column.shape), column.dtype)
    full = put(full, column, zl)
    for by in (1, -1):
        block = shift_z(column, by)
        full = put(full, block, jnp.mod(zl - by + NZL, NZL))
    far_low = shift_z(column[: NY // 2], 2)
    far_high = shift_z(column[NY // 2 :], -2)
    far = jnp.concatenate((far_low, far_high), axis=0)
    return put(full, far, jnp.mod(zl + 2, NZL))


def reduce_on_tp(late, early, x, c):
    n_x = lax.axis_size("x")
    tokens, width = late.shape
    cut = lambda a: a.reshape(n_x, 2, tokens // (2 * n_x), width)
    both = jnp.concatenate((cut(late), cut(early)), axis=2)
    pick = lambda at: lax.dynamic_index_in_dim(both, at, 1, keepdims=False)
    other = lax.ppermute(pick(1 - c), "c", [(0, 1), (1, 0)])
    pair = (pick(c).astype(jnp.float32) + other.astype(jnp.float32)).astype(late.dtype)
    part = lambda at: lax.dynamic_index_in_dim(pair, at, 0, keepdims=False)
    total = part(x).astype(jnp.float32)
    for by in (1, -1, 2):
        block = part(jnp.mod(x + by + n_x, n_x))
        sent = shift(block, "x", n_x, by)
        total = total + sent.astype(jnp.float32)
    return total.astype(late.dtype)


def everywhere_on_tp(own, x, c):
    n_x = lax.axis_size("x")
    line = jnp.zeros((n_x, *own.shape), own.dtype)
    line = put(line, own, x)
    for by in (1, -1, 2):
        line = put(line, shift(own, "x", n_x, by), jnp.mod(x - by + n_x, n_x))
    other = lax.ppermute(line, "c", [(0, 1), (1, 0)])
    both = jnp.zeros((n_x, 2, *own.shape), own.dtype)
    both = put(both, line, c, 1)
    both = put(both, other, 1 - c, 1)
    return both.reshape(2 * n_x, *own.shape)


def per_device(
    later_input,
    earlier_input,
    cotangent,
    gate_weight,
    up_weight,
    down_weight,
    gate_sum,
    up_sum,
    down_sum,
):
    bf = jnp.bfloat16
    zl = lax.axis_index("zl")
    rows, width = gate_weight.shape
    part_b = gather_y_then_z((up_weight, down_weight), zl).reshape(-1, 2 * width)
    gate_full = gather_z_then_y(gate_weight, zl).reshape(-1, width)
    up_full = part_b[:, :width]
    down_full = part_b[:, width:]

    block = rows * NY

    def features_for(where):
        cut = lambda a: lax.dynamic_slice_in_dim(a, where * block, block, 1)
        return jnp.concatenate((cut(earlier_input), cut(cotangent)), axis=1)

    features = [features_for(zl)]
    for by in SHIFTS:
        sent = features_for(jnp.mod(zl + by + NZL, NZL))
        features.append(shift_z(sent, by))

    gate_early = dot(earlier_input, gate_full)
    up_early = dot(earlier_input, up_full)
    hidden_grad = dot(cotangent, down_full)
    sigmoid_gate = jax.nn.sigmoid(gate_early)
    silu_early = gate_early * sigmoid_gate
    gate_grad = (
        hidden_grad * up_early * sigmoid_gate * (1.0 + gate_early * (1.0 - sigmoid_gate))
    ).astype(bf)
    up_grad = (hidden_grad * silu_early).astype(bf)
    hidden_early = (silu_early * up_early).astype(bf)

    piece = jnp.concatenate((gate_grad, up_grad, hidden_early), axis=1)
    pieces = [piece]
    for by in SHIFTS:
        pieces.append(shift_z(piece, by))

    gate_late = dot(later_input, gate_full)
    up_late = dot(later_input, up_full)
    hidden_late = (jax.nn.silu(gate_late) * up_late).astype(bf)
    partial_late = contract_last(hidden_late, down_full).astype(bf)
    partial_early = (
        contract_last(gate_grad, gate_full) + contract_last(up_grad, up_full)
    ).astype(bf)
    tokens = partial_late.shape[0]
    n_tp = lax.axis_size(TP)
    x, c = lax.axis_index("x"), lax.axis_index("c")
    own = reduce_on_tp(partial_late, partial_early, x, c)
    outs = everywhere_on_tp(own, x, c)
    later_output = outs[:, : tokens // n_tp].reshape(tokens, -1)
    earlier_input_grad = outs[:, tokens // n_tp :].reshape(tokens, -1)

    first = jnp.concatenate(features, axis=0)
    second = jnp.concatenate(pieces, axis=0)
    both_local = contract_first(first[:, :block], second[:, : 2 * width])
    down_local = contract_first(first[:, block:], second[:, 2 * width :])
    local = jnp.concatenate((both_local.astype(bf), down_local.astype(bf)), axis=1)
    local = local.reshape(NY, rows, 3 * width)
    local = lax.all_to_all(local, "y", split_axis=0, concat_axis=0, tiled=True)
    mine = jnp.sum(local.astype(jnp.float32), axis=0).astype(bf)
    other = lax.ppermute(mine, "zh", [(0, 1), (1, 0)])
    total = mine.astype(jnp.float32) + other.astype(jnp.float32)
    return (
        later_output,
        earlier_input_grad,
        gate_sum + total[:, :width],
        up_sum + total[:, width : 2 * width],
        down_sum + total[:, 2 * width :],
    )


def solution(mesh):
    fine = Mesh(mesh.devices.reshape(2, NZL, NY, -1, 2), ("zh", "zl", "y", "x", "c"))
    tokens = P(("zh", "zl", "y"), None)
    weights = P(("zl", "y"), ("x", "c"))
    return jax.shard_map(
        per_device,
        mesh=fine,
        in_specs=(tokens,) * 3 + (weights,) * 6,
        out_specs=(tokens,) * 2 + (weights,) * 3,
        check_vma=False,
    )
```

```python
import jax
import jax.numpy as jnp
from jax import lax
from jax.sharding import Mesh, PartitionSpec as P


NZ = 8
NZL = 4
NY = 8
RING = ("zh", "zl")
TP = ("x", "c")
SHIFTS = (1, -1, -2)


def shift_z(array, by):
    return lax.ppermute(array, RING, [(i, (i + by) % NZ) for i in range(NZ)])


def contract_last(first, second):
    return lax.dot_general(
        first, second, (((1,), (1,)), ((), ())), preferred_element_type=jnp.float32
    )


def contract_first(first, second):
    return lax.dot_general(
        first, second, (((0,), (0,)), ((), ())), preferred_element_type=jnp.float32
    )


def dot(first, second):
    return jnp.dot(first, second, preferred_element_type=jnp.float32)


def shift(array, axis, count, by):
    return lax.ppermute(array, axis, [(i, (i + by) % count) for i in range(count)])


def put(buffer, block, at, dim=0):
    return lax.dynamic_update_slice_in_dim(buffer, jnp.expand_dims(block, dim), at, dim)


def spread_y(block):
    return lax.all_to_all(block, "y", split_axis=0, concat_axis=0, tiled=True)


def gather_z_then_y(shard, zl):
    near = jnp.zeros((NZL, *shard.shape), shard.dtype)
    near = put(near, shard, zl)
    for by in SHIFTS:
        block = shift_z(shard, by)
        near = put(near, block, jnp.mod(zl - by + NZL, NZL))
    full = spread_y(jnp.broadcast_to(near, (NY, *near.shape)))
    return full.transpose(1, 0, 2, 3)


def gather_y_then_z(shards, zl):
    shard = jnp.concatenate(shards, axis=1)
    column = spread_y(jnp.broadcast_to(shard, (NY, *shard.shape)))
    full = jnp.zeros((NZL, *column.shape), column.dtype)
    full = put(full, column, zl)
    for by in (1, -1):
        block = shift_z(column, by)
        full = put(full, block, jnp.mod(zl - by + NZL, NZL))
    far_low = shift_z(column[: NY // 2], 2)
    far_high = shift_z(column[NY // 2 :], -2)
    far = jnp.concatenate((far_low, far_high), axis=0)
    return put(full, far, jnp.mod(zl + 2, NZL))


def reduce_on_tp(late, early, x, c):
    n_x = lax.axis_size("x")
    tokens, width = late.shape
    cut = lambda a: a.reshape(n_x, 2, tokens // (2 * n_x), width)
    both = jnp.concatenate((cut(late), cut(early)), axis=2)
    pick = lambda at: lax.dynamic_index_in_dim(both, at, 1, keepdims=False)
    other = lax.ppermute(pick(1 - c), "c", [(0, 1), (1, 0)])
    pair = (pick(c).astype(jnp.float32) + other.astype(jnp.float32)).astype(late.dtype)
    part = lambda at: lax.dynamic_index_in_dim(pair, at, 0, keepdims=False)
    total = part(x).astype(jnp.float32)
    for by in (1, -1, 2):
        block = part(jnp.mod(x + by + n_x, n_x))
        sent = shift(block, "x", n_x, by)
        total = total + sent.astype(jnp.float32)
    return total.astype(late.dtype)


def everywhere_on_tp(own, x, c):
    n_x = lax.axis_size("x")
    line = jnp.zeros((n_x, *own.shape), own.dtype)
    line = put(line, own, x)
    for by in (1, -1, 2):
        block = shift(own, "x", n_x, by)
        line = put(line, block, jnp.mod(x - by + n_x, n_x))
    other = lax.ppermute(line, "c", [(0, 1), (1, 0)])
    both = jnp.zeros((n_x, 2, *own.shape), own.dtype)
    both = put(both, line, c, 1)
    both = put(both, other, 1 - c, 1)
    return both.reshape(2 * n_x, *own.shape)


def per_device(
    later_input,
    earlier_input,
    cotangent,
    gate_weight,
    up_weight,
    down_weight,
    gate_sum,
    up_sum,
    down_sum,
):
    bf = jnp.bfloat16
    zl = lax.axis_index("zl")
    rows, width = gate_weight.shape
    part_b = gather_y_then_z((up_weight, down_weight), zl).reshape(-1, 2 * width)
    gate_full = gather_z_then_y(gate_weight, zl).reshape(-1, width)
    up_full = part_b[:, :width]
    down_full = part_b[:, width:]

    block = rows * NY

    def features_for(where):
        cut = lambda a: lax.dynamic_slice_in_dim(a, where * block, block, 1)
        return jnp.concatenate((cut(earlier_input), cut(cotangent)), axis=1)

    features = [features_for(zl)]
    c = lax.axis_index("c")
    halves = []
    for k, by in enumerate(SHIFTS):
        sent = features_for(jnp.mod(zl + by + NZL, NZL))
        if k:
            tokens_half = sent.shape[0] // 2
            sent = lax.dynamic_slice_in_dim(sent, c * tokens_half, tokens_half, 0)
        arrived = shift_z(sent, by)
        (halves if k else features).append(arrived)
    halves = jnp.stack(halves)
    others = lax.ppermute(halves, "c", [(0, 1), (1, 0)])
    far = jnp.zeros((halves.shape[0], 2, *halves.shape[1:]), halves.dtype)
    far = put(put(far, halves, c, 1), others, 1 - c, 1)
    features += [f.reshape(-1, f.shape[-1]) for f in far]

    gate_early = dot(earlier_input, gate_full)
    up_early = dot(earlier_input, up_full)
    hidden_grad = dot(cotangent, down_full)
    sigmoid_gate = jax.nn.sigmoid(gate_early)
    silu_early = gate_early * sigmoid_gate
    gate_grad = (
        hidden_grad * up_early * sigmoid_gate * (1.0 + gate_early * (1.0 - sigmoid_gate))
    ).astype(bf)
    up_grad = (hidden_grad * silu_early).astype(bf)
    hidden_early = (silu_early * up_early).astype(bf)

    piece = jnp.concatenate((gate_grad, up_grad, hidden_early), axis=1)
    pieces = [piece]
    for by in SHIFTS:
        pieces.append(shift_z(piece, by))

    gate_late = dot(later_input, gate_full)
    up_late = dot(later_input, up_full)
    hidden_late = (jax.nn.silu(gate_late) * up_late).astype(bf)
    partial_late = contract_last(hidden_late, down_full).astype(bf)
    partial_early = (
        contract_last(gate_grad, gate_full) + contract_last(up_grad, up_full)
    ).astype(bf)
    tokens = partial_late.shape[0]
    n_tp = lax.axis_size(TP)
    x = lax.axis_index("x")
    own = reduce_on_tp(partial_late, partial_early, x, c)
    outs = everywhere_on_tp(own, x, c)
    later_output = outs[:, : tokens // n_tp].reshape(tokens, -1)
    earlier_input_grad = outs[:, tokens // n_tp :].reshape(tokens, -1)

    first = jnp.concatenate(features, axis=0)
    second = jnp.concatenate(pieces, axis=0)
    both_local = contract_first(first[:, :block], second[:, : 2 * width])
    down_local = contract_first(first[:, block:], second[:, 2 * width :])
    local = jnp.concatenate((both_local.astype(bf), down_local.astype(bf)), axis=1)
    local = local.reshape(NY, rows, 3 * width)
    local = lax.all_to_all(local, "y", split_axis=0, concat_axis=0, tiled=True)
    mine = jnp.sum(local.astype(jnp.float32), axis=0).astype(bf)
    other = lax.ppermute(mine, "zh", [(0, 1), (1, 0)])
    total = mine.astype(jnp.float32) + other.astype(jnp.float32)
    return (
        later_output,
        earlier_input_grad,
        gate_sum + total[:, :width],
        up_sum + total[:, width : 2 * width],
        down_sum + total[:, 2 * width :],
    )


def solution(mesh):
    fine = Mesh(mesh.devices.reshape(2, NZL, NY, -1, 2), ("zh", "zl", "y", "x", "c"))
    tokens = P(("zh", "zl", "y"), None)
    weights = P(("zl", "y"), ("x", "c"))
    return jax.shard_map(
        per_device,
        mesh=fine,
        in_specs=(tokens,) * 3 + (weights,) * 6,
        out_specs=(tokens,) * 2 + (weights,) * 3,
        check_vma=False,
    )
```

```python
import jax
import jax.numpy as jnp
from jax import lax
from jax.sharding import Mesh, PartitionSpec as P


NZ = 8
NZL = 4
NY = 8
RING = ("zh", "zl")
TP = ("x", "c")
SHIFTS = (1, -1, -2)


def shift_z(array, by):
    return lax.ppermute(array, RING, [(i, (i + by) % NZ) for i in range(NZ)])


def contract_last(first, second):
    return lax.dot_general(
        first, second, (((1,), (1,)), ((), ())), preferred_element_type=jnp.float32
    )


def contract_first(first, second):
    return lax.dot_general(
        first, second, (((0,), (0,)), ((), ())), preferred_element_type=jnp.float32
    )


def dot(first, second):
    return jnp.dot(first, second, preferred_element_type=jnp.float32)


def shift(array, axis, count, by):
    return lax.ppermute(array, axis, [(i, (i + by) % count) for i in range(count)])


def put(buffer, block, at, dim=0):
    return lax.dynamic_update_slice_in_dim(buffer, jnp.expand_dims(block, dim), at, dim)


def spread_y(block):
    return lax.all_to_all(block, "y", split_axis=0, concat_axis=0, tiled=True)


def gather_z_then_y(shard, zl):
    near = jnp.zeros((NZL, *shard.shape), shard.dtype)
    near = put(near, shard, zl)
    for by in SHIFTS:
        block = shift_z(shard, by)
        near = put(near, block, jnp.mod(zl - by + NZL, NZL))
    full = spread_y(jnp.broadcast_to(near, (NY, *near.shape)))
    return full.transpose(1, 0, 2, 3)


def gather_y_then_z(shards, zl):
    shard = jnp.concatenate(shards, axis=1)
    column = spread_y(jnp.broadcast_to(shard, (NY, *shard.shape)))
    full = jnp.zeros((NZL, *column.shape), column.dtype)
    full = put(full, column, zl)
    for by in (1, -1):
        block = shift_z(column, by)
        full = put(full, block, jnp.mod(zl - by + NZL, NZL))
    far_low = shift_z(column[: NY // 2], 2)
    far_high = shift_z(column[NY // 2 :], -2)
    return full, far_low, far_high


def reduce_on_tp(late, early, x, c):
    n_x = lax.axis_size("x")
    tokens, width = late.shape
    cut = lambda a: a.reshape(n_x, 2, tokens // (2 * n_x), width)
    both = jnp.concatenate((cut(late), cut(early)), axis=2)
    pick = lambda at: lax.dynamic_index_in_dim(both, at, 1, keepdims=False)
    other = lax.ppermute(pick(1 - c), "c", [(0, 1), (1, 0)])
    pair = (pick(c).astype(jnp.float32) + other.astype(jnp.float32)).astype(late.dtype)
    part = lambda at: lax.dynamic_index_in_dim(pair, at, 0, keepdims=False)
    total = part(x).astype(jnp.float32)
    for by in (1, -1, 2):
        block = part(jnp.mod(x + by + n_x, n_x))
        sent = shift(block, "x", n_x, by)
        total = total + sent.astype(jnp.float32)
    return total.astype(late.dtype)


def everywhere_on_tp(own, x, c):
    n_x = lax.axis_size("x")
    line = jnp.zeros((n_x, *own.shape), own.dtype)
    line = put(line, own, x)
    for by in (1, -1, 2):
        block = shift(own, "x", n_x, by)
        line = put(line, block, jnp.mod(x - by + n_x, n_x))
    other = lax.ppermute(line, "c", [(0, 1), (1, 0)])
    both = jnp.zeros((n_x, 2, *own.shape), own.dtype)
    both = put(both, line, c, 1)
    both = put(both, other, 1 - c, 1)
    return both.reshape(2 * n_x, *own.shape)


def per_device(
    later_input,
    earlier_input,
    cotangent,
    gate_weight,
    up_weight,
    down_weight,
    gate_sum,
    up_sum,
    down_sum,
):
    bf = jnp.bfloat16
    zl = lax.axis_index("zl")
    rows, width = gate_weight.shape
    near, far_low, far_high = gather_y_then_z((up_weight, down_weight), zl)
    far = jnp.concatenate((far_low, far_high), axis=0)
    far_at = jnp.mod(zl + 2, NZL)
    part_b = put(near, far, far_at).reshape(-1, 2 * width)
    gate_full = gather_z_then_y(gate_weight, zl).reshape(-1, width)
    up_full = part_b[:, :width]
    down_full = part_b[:, width:]

    block = rows * NY

    def features_for(where):
        cut = lambda a: lax.dynamic_slice_in_dim(a, where * block, block, 1)
        return jnp.concatenate((cut(earlier_input), cut(cotangent)), axis=1)

    features = [features_for(zl)]
    c = lax.axis_index("c")
    halves = []
    for k, by in enumerate(SHIFTS):
        sent = features_for(jnp.mod(zl + by + NZL, NZL))
        if k:
            tokens_half = sent.shape[0] // 2
            sent = lax.dynamic_slice_in_dim(sent, c * tokens_half, tokens_half, 0)
        arrived = shift_z(sent, by)
        (halves if k else features).append(arrived)
    halves = jnp.stack(halves)
    others = lax.ppermute(halves, "c", [(0, 1), (1, 0)])
    far = jnp.zeros((halves.shape[0], 2, *halves.shape[1:]), halves.dtype)
    far = put(put(far, halves, c, 1), others, 1 - c, 1)
    features += [f.reshape(-1, f.shape[-1]) for f in far]

    near_rows = near.reshape(-1, 2 * width)
    near_up = dot(earlier_input, near_rows[:, :width])
    near_grad = dot(cotangent, near_rows[:, width:])
    gate_early = dot(earlier_input, gate_full)
    near_up, near_grad = lax.optimization_barrier((near_up, near_grad))
    low = far_low.reshape(-1, 2 * width)
    high = far_high.reshape(-1, 2 * width)
    far_x, far_cot = jnp.split(features_for(far_at), 2, axis=1)

    def with_far(total, array, at):
        n = low.shape[0]
        total = total + dot(array[:, :n], low[:, at : at + width])
        return total + dot(array[:, n:], high[:, at : at + width])

    up_early = with_far(near_up, far_x, 0)
    hidden_grad = with_far(near_grad, far_cot, width)
    sigmoid_gate = jax.nn.sigmoid(gate_early)
    silu_early = gate_early * sigmoid_gate
    gate_grad = (
        hidden_grad * up_early * sigmoid_gate * (1.0 + gate_early * (1.0 - sigmoid_gate))
    ).astype(bf)
    up_grad = (hidden_grad * silu_early).astype(bf)
    hidden_early = (silu_early * up_early).astype(bf)

    piece = jnp.concatenate((gate_grad, up_grad, hidden_early), axis=1)
    pieces = [piece]
    for by in SHIFTS:
        pieces.append(shift_z(piece, by))

    gate_late = dot(later_input, gate_full)
    up_late = dot(later_input, up_full)
    hidden_late = (jax.nn.silu(gate_late) * up_late).astype(bf)
    partial_late = contract_last(hidden_late, down_full).astype(bf)
    partial_early = (
        contract_last(gate_grad, gate_full) + contract_last(up_grad, up_full)
    ).astype(bf)
    tokens = partial_late.shape[0]
    n_tp = lax.axis_size(TP)
    x = lax.axis_index("x")
    own = reduce_on_tp(partial_late, partial_early, x, c)
    outs = everywhere_on_tp(own, x, c)
    later_output = outs[:, : tokens // n_tp].reshape(tokens, -1)
    earlier_input_grad = outs[:, tokens // n_tp :].reshape(tokens, -1)

    first = jnp.concatenate(features, axis=0)
    second = jnp.concatenate(pieces, axis=0)
    both_local = contract_first(first[:, :block], second[:, : 2 * width])
    down_local = contract_first(first[:, block:], second[:, 2 * width :])
    local = jnp.concatenate((both_local.astype(bf), down_local.astype(bf)), axis=1)
    local = local.reshape(NY, rows, 3 * width)
    local = lax.all_to_all(local, "y", split_axis=0, concat_axis=0, tiled=True)
    mine = jnp.sum(local.astype(jnp.float32), axis=0).astype(bf)
    other = lax.ppermute(mine, "zh", [(0, 1), (1, 0)])
    total = mine.astype(jnp.float32) + other.astype(jnp.float32)
    return (
        later_output,
        earlier_input_grad,
        gate_sum + total[:, :width],
        up_sum + total[:, width : 2 * width],
        down_sum + total[:, 2 * width :],
    )


def solution(mesh):
    fine = Mesh(mesh.devices.reshape(2, NZL, NY, -1, 2), ("zh", "zl", "y", "x", "c"))
    tokens = P(("zh", "zl", "y"), None)
    weights = P(("zl", "y"), ("x", "c"))
    return jax.shard_map(
        per_device,
        mesh=fine,
        in_specs=(tokens,) * 3 + (weights,) * 6,
        out_specs=(tokens,) * 2 + (weights,) * 3,
        check_vma=False,
    )
```

```python
import jax
import jax.numpy as jnp
from jax import lax
from jax.sharding import Mesh, PartitionSpec as P


NZ = 8
NZL = 4
NY = 8
RING = ("zh", "zl")
TP = ("x", "c")
SHIFTS = (1, -1, -2)


def shift_z(array, by):
    return lax.ppermute(array, RING, [(i, (i + by) % NZ) for i in range(NZ)])


def contract_last(first, second):
    return lax.dot_general(
        first, second, (((1,), (1,)), ((), ())), preferred_element_type=jnp.float32
    )


def contract_first(first, second):
    return lax.dot_general(
        first, second, (((0,), (0,)), ((), ())), preferred_element_type=jnp.float32
    )


def dot(first, second):
    return jnp.dot(first, second, preferred_element_type=jnp.float32)


def shift(array, axis, count, by):
    return lax.ppermute(array, axis, [(i, (i + by) % count) for i in range(count)])


def put(buffer, block, at, dim=0):
    return lax.dynamic_update_slice_in_dim(buffer, jnp.expand_dims(block, dim), at, dim)


def spread_y(block):
    return lax.all_to_all(block, "y", split_axis=0, concat_axis=0, tiled=True)


def gather_z_then_y(shard, zl):
    near = jnp.zeros((NZL, *shard.shape), shard.dtype)
    near = put(near, shard, zl)
    for by in SHIFTS:
        block = shift_z(shard, by)
        near = put(near, block, jnp.mod(zl - by + NZL, NZL))
    full = spread_y(jnp.broadcast_to(near, (NY, *near.shape)))
    return full.transpose(1, 0, 2, 3)


def gather_y_then_z(shards, zl):
    shard = jnp.concatenate(shards, axis=1)
    column = spread_y(jnp.broadcast_to(shard, (NY, *shard.shape)))
    full = jnp.zeros((NZL, *column.shape), column.dtype)
    full = put(full, column, zl)
    for by in (1, -1):
        block = shift_z(column, by)
        full = put(full, block, jnp.mod(zl - by + NZL, NZL))
    far_low = shift_z(column[: NY // 2], 2)
    far_high = shift_z(column[NY // 2 :], -2)
    return full, far_low, far_high


def reduce_on_tp(late, early, x, c):
    n_x = lax.axis_size("x")
    tokens, width = late.shape
    cut = lambda a: a.reshape(n_x, 2, tokens // (2 * n_x), width)
    both = jnp.concatenate((cut(late), cut(early)), axis=2)
    pick = lambda at: lax.dynamic_index_in_dim(both, at, 1, keepdims=False)
    other = lax.ppermute(pick(1 - c), "c", [(0, 1), (1, 0)])
    pair = (pick(c).astype(jnp.float32) + other.astype(jnp.float32)).astype(late.dtype)
    part = lambda at: lax.dynamic_index_in_dim(pair, at, 0, keepdims=False)
    total = part(x).astype(jnp.float32)
    for by in (1, -1, 2):
        block = part(jnp.mod(x + by + n_x, n_x))
        sent = shift(block, "x", n_x, by)
        total = total + sent.astype(jnp.float32)
    return total.astype(late.dtype)


def everywhere_on_tp(own, x, c):
    n_x = lax.axis_size("x")
    line = jnp.zeros((n_x, *own.shape), own.dtype)
    line = put(line, own, x)
    for by in (1, -1, 2):
        block = shift(own, "x", n_x, by)
        line = put(line, block, jnp.mod(x - by + n_x, n_x))
    other = lax.ppermute(line, "c", [(0, 1), (1, 0)])
    both = jnp.zeros((n_x, 2, *own.shape), own.dtype)
    both = put(both, line, c, 1)
    both = put(both, other, 1 - c, 1)
    return both.reshape(2 * n_x, *own.shape)


def per_device(
    later_input,
    earlier_input,
    cotangent,
    gate_weight,
    up_weight,
    down_weight,
    gate_sum,
    up_sum,
    down_sum,
):
    bf = jnp.bfloat16
    zl = lax.axis_index("zl")
    rows, width = gate_weight.shape
    near, far_low, far_high = gather_y_then_z((up_weight, down_weight), zl)
    far = jnp.concatenate((far_low, far_high), axis=0)
    far_at = jnp.mod(zl + 2, NZL)
    part_b = put(near, far, far_at).reshape(-1, 2 * width)
    gate_full = gather_z_then_y(gate_weight, zl).reshape(-1, width)
    up_full = part_b[:, :width]
    down_full = part_b[:, width:]

    block = rows * NY

    def features_for(where):
        cut = lambda a: lax.dynamic_slice_in_dim(a, where * block, block, 1)
        return jnp.concatenate((cut(earlier_input), cut(cotangent)), axis=1)

    features = [features_for(zl)]
    for by in SHIFTS:
        sent = features_for(jnp.mod(zl + by + NZL, NZL))
        features.append(shift_z(sent, by))

    near_rows = near.reshape(-1, 2 * width)
    near_up = dot(earlier_input, near_rows[:, :width])
    near_grad = dot(cotangent, near_rows[:, width:])
    gate_early = dot(earlier_input, gate_full)
    far_x, far_cot = jnp.split(features_for(far_at), 2, axis=1)
    near_up, near_grad, far_x, far_cot = lax.optimization_barrier(
        (near_up, near_grad, far_x, far_cot)
    )
    low = far_low.reshape(-1, 2 * width)
    high = far_high.reshape(-1, 2 * width)

    def with_far(total, array, at):
        n = low.shape[0]
        total = total + dot(array[:, :n], low[:, at : at + width])
        return total + dot(array[:, n:], high[:, at : at + width])

    up_early = with_far(near_up, far_x, 0)
    hidden_grad = with_far(near_grad, far_cot, width)
    sigmoid_gate = jax.nn.sigmoid(gate_early)
    silu_early = gate_early * sigmoid_gate
    gate_grad = (
        hidden_grad * up_early * sigmoid_gate * (1.0 + gate_early * (1.0 - sigmoid_gate))
    ).astype(bf)
    up_grad = (hidden_grad * silu_early).astype(bf)
    hidden_early = (silu_early * up_early).astype(bf)

    piece = jnp.concatenate((gate_grad, up_grad, hidden_early), axis=1)
    pieces = [piece]
    for by in SHIFTS:
        pieces.append(shift_z(piece, by))

    gate_late = dot(later_input, gate_full)
    up_late = dot(later_input, up_full)
    hidden_late = (jax.nn.silu(gate_late) * up_late).astype(bf)
    partial_late = contract_last(hidden_late, down_full).astype(bf)
    partial_early = (
        contract_last(gate_grad, gate_full) + contract_last(up_grad, up_full)
    ).astype(bf)
    tokens = partial_late.shape[0]
    n_tp = lax.axis_size(TP)
    x, c = lax.axis_index("x"), lax.axis_index("c")
    own = reduce_on_tp(partial_late, partial_early, x, c)
    outs = everywhere_on_tp(own, x, c)
    later_output = outs[:, : tokens // n_tp].reshape(tokens, -1)
    earlier_input_grad = outs[:, tokens // n_tp :].reshape(tokens, -1)

    first = jnp.concatenate(features, axis=0)
    second = jnp.concatenate(pieces, axis=0)
    both_local = contract_first(first[:, :block], second[:, : 2 * width])
    down_local = contract_first(first[:, block:], second[:, 2 * width :])
    local = jnp.concatenate((both_local.astype(bf), down_local.astype(bf)), axis=1)
    local = local.reshape(NY, rows, 3 * width)
    local = lax.all_to_all(local, "y", split_axis=0, concat_axis=0, tiled=True)
    mine = jnp.sum(local.astype(jnp.float32), axis=0).astype(bf)
    other = lax.ppermute(mine, "zh", [(0, 1), (1, 0)])
    total = mine.astype(jnp.float32) + other.astype(jnp.float32)
    return (
        later_output,
        earlier_input_grad,
        gate_sum + total[:, :width],
        up_sum + total[:, width : 2 * width],
        down_sum + total[:, 2 * width :],
    )


def solution(mesh):
    fine = Mesh(mesh.devices.reshape(2, NZL, NY, -1, 2), ("zh", "zl", "y", "x", "c"))
    tokens = P(("zh", "zl", "y"), None)
    weights = P(("zl", "y"), ("x", "c"))
    return jax.shard_map(
        per_device,
        mesh=fine,
        in_specs=(tokens,) * 3 + (weights,) * 6,
        out_specs=(tokens,) * 2 + (weights,) * 3,
        check_vma=False,
    )
```

```python
import functools

import jax
import jax.numpy as jnp
from jax import lax
from jax.experimental import pallas as pl
from jax.sharding import Mesh, PartitionSpec as P


NZ = 8
NZL = 4
NY = 8
RING = ("zh", "zl")
TP = ("x", "c")
SHIFTS = (1, -1, -2)


def shift_z(array, by):
    return lax.ppermute(array, RING, [(i, (i + by) % NZ) for i in range(NZ)])


def contract_last(first, second):
    return lax.dot_general(
        first, second, (((1,), (1,)), ((), ())), preferred_element_type=jnp.float32
    )


def contract_first(first, second):
    return lax.dot_general(
        first, second, (((0,), (0,)), ((), ())), preferred_element_type=jnp.float32
    )


def dot(first, second):
    return jnp.dot(first, second, preferred_element_type=jnp.float32)


def shift(array, axis, count, by):
    return lax.ppermute(array, axis, [(i, (i + by) % count) for i in range(count)])


def put(buffer, block, at, dim=0):
    return lax.dynamic_update_slice_in_dim(buffer, jnp.expand_dims(block, dim), at, dim)


def spread_y(block):
    return lax.all_to_all(block, "y", split_axis=0, concat_axis=0, tiled=True)


def gather_z_then_y(shard, zl):
    near = jnp.zeros((NZL, *shard.shape), shard.dtype)
    near = put(near, shard, zl)
    for by in SHIFTS:
        block = shift_z(shard, by)
        near = put(near, block, jnp.mod(zl - by + NZL, NZL))
    full = spread_y(jnp.broadcast_to(near, (NY, *near.shape)))
    return full.transpose(1, 0, 2, 3)


def gather_y_then_z(shards, zl):
    shard = jnp.concatenate(shards, axis=1)
    column = spread_y(jnp.broadcast_to(shard, (NY, *shard.shape)))
    full = jnp.zeros((NZL, *column.shape), column.dtype)
    full = put(full, column, zl)
    for by in (1, -1):
        block = shift_z(column, by)
        full = put(full, block, jnp.mod(zl - by + NZL, NZL))
    far_low = shift_z(column[: NY // 2], 2)
    far_high = shift_z(column[NY // 2 :], -2)
    return full, far_low, far_high


def reduce_on_tp(late, early, x, c):
    n_x = lax.axis_size("x")
    tokens, width = late.shape
    cut = lambda a: a.reshape(n_x, 2, tokens // (2 * n_x), width)
    both = jnp.concatenate((cut(late), cut(early)), axis=2)
    pick = lambda at: lax.dynamic_index_in_dim(both, at, 1, keepdims=False)
    other = lax.ppermute(pick(1 - c), "c", [(0, 1), (1, 0)])
    pair = (pick(c).astype(jnp.float32) + other.astype(jnp.float32)).astype(late.dtype)
    part = lambda at: lax.dynamic_index_in_dim(pair, at, 0, keepdims=False)
    total = part(x).astype(jnp.float32)
    for by in (1, -1, 2):
        block = part(jnp.mod(x + by + n_x, n_x))
        sent = shift(block, "x", n_x, by)
        total = total + sent.astype(jnp.float32)
    return total.astype(late.dtype)


def everywhere_on_tp(own, x, c):
    n_x = lax.axis_size("x")
    line = jnp.zeros((n_x, *own.shape), own.dtype)
    line = put(line, own, x)
    for by in (1, -1, 2):
        block = shift(own, "x", n_x, by)
        line = put(line, block, jnp.mod(x - by + n_x, n_x))
    other = lax.ppermute(line, "c", [(0, 1), (1, 0)])
    both = jnp.zeros((n_x, 2, *own.shape), own.dtype)
    both = put(both, line, c, 1)
    both = put(both, other, 1 - c, 1)
    return both.reshape(2 * n_x, *own.shape)


def early_kernel(gate, near_up, near_grad, far_x, far_cot, low, high, out):
    n, width = low.shape[0], gate.shape[1]

    def full(near, far, at):
        cols = slice(at, at + width)
        return (
            near[...] + dot(far[:, :n], low[:, cols]) + dot(far[:, n:], high[:, cols])
        )

    g = gate[...]
    up = full(near_up, far_x, 0)
    grad = full(near_grad, far_cot, width)
    s = jax.nn.sigmoid(g)
    silu = g * s
    out[:, :width] = (grad * up * s * (1.0 + g * (1.0 - s))).astype(out.dtype)
    out[:, width : 2 * width] = (grad * silu).astype(out.dtype)
    out[:, 2 * width :] = (silu * up).astype(out.dtype)


def early_piece(*arrays):
    tokens, width = arrays[0].shape
    return pl.pallas_call(
        early_kernel,
        out_shape=jax.ShapeDtypeStruct((tokens, 3 * width), jnp.bfloat16),
        cost_estimate=pl.CostEstimate(
            flops=800_000_000, bytes_accessed=2_600_000, transcendentals=50_000
        ),
    )(*arrays)


def grads_kernel(count, *refs):
    x, cot, pieces, out = (
        refs[:count],
        refs[count : 2 * count],
        refs[2 * count : 3 * count],
        refs[3 * count],
    )
    cut = out.shape[1] * 2 // 3
    both = sum(contract_first(a[...], p[:, :cut]) for a, p in zip(x, pieces))
    out[:, :cut] = both.astype(out.dtype)
    down = sum(contract_first(a[...], p[:, cut:]) for a, p in zip(cot, pieces))
    out[:, cut:] = down.astype(out.dtype)


def local_grads(features, pieces):
    count, (tokens, columns) = len(features), features[0].shape
    rows, width = columns // 2, pieces[0].shape[1]
    step = 128
    steps = rows // step
    return pl.pallas_call(
        functools.partial(grads_kernel, count),
        grid=(steps,),
        in_specs=[pl.BlockSpec((tokens, step), lambda i: (0, i))] * count
        + [pl.BlockSpec((tokens, step), lambda i: (0, steps + i))] * count
        + [pl.BlockSpec((tokens, width), lambda i: (0, 0))] * count,
        out_specs=pl.BlockSpec((step, width), lambda i: (i, 0)),
        out_shape=jax.ShapeDtypeStruct((rows, width), jnp.bfloat16),
        cost_estimate=pl.CostEstimate(
            flops=1_200_000_000, bytes_accessed=3_400_000, transcendentals=0
        ),
    )(*features, *features, *pieces)


def per_device(
    later_input,
    earlier_input,
    cotangent,
    gate_weight,
    up_weight,
    down_weight,
    gate_sum,
    up_sum,
    down_sum,
):
    bf = jnp.bfloat16
    zl = lax.axis_index("zl")
    rows, width = gate_weight.shape
    near, far_low, far_high = gather_y_then_z((up_weight, down_weight), zl)
    far = jnp.concatenate((far_low, far_high), axis=0)
    far_at = jnp.mod(zl + 2, NZL)
    part_b = put(near, far, far_at).reshape(-1, 2 * width)
    gate_full = gather_z_then_y(gate_weight, zl).reshape(-1, width)
    up_full = part_b[:, :width]
    down_full = part_b[:, width:]

    block = rows * NY

    def features_for(where):
        cut = lambda a: lax.dynamic_slice_in_dim(a, where * block, block, 1)
        return jnp.concatenate((cut(earlier_input), cut(cotangent)), axis=1)

    features = [features_for(zl)]
    for by in SHIFTS:
        sent = features_for(jnp.mod(zl + by + NZL, NZL))
        features.append(shift_z(sent, by))

    near_rows = near.reshape(-1, 2 * width)
    near_up = dot(earlier_input, near_rows[:, :width])
    near_grad = dot(cotangent, near_rows[:, width:])
    gate_early = dot(earlier_input, gate_full)
    far_x, far_cot = jnp.split(features_for(far_at), 2, axis=1)
    near_up, near_grad, far_x, far_cot = lax.optimization_barrier(
        (near_up, near_grad, far_x, far_cot)
    )
    low = far_low.reshape(-1, 2 * width)
    high = far_high.reshape(-1, 2 * width)

    piece = early_piece(
        gate_early, near_up, near_grad, far_x, far_cot, low, high
    )
    gate_grad = piece[:, :width]
    up_grad = piece[:, width : 2 * width]

    pieces = [piece]
    for by in SHIFTS:
        pieces.append(shift_z(piece, by))

    gate_late = dot(later_input, gate_full)
    up_late = dot(later_input, up_full)
    hidden_late = (jax.nn.silu(gate_late) * up_late).astype(bf)
    partial_late = contract_last(hidden_late, down_full).astype(bf)
    partial_early = (
        contract_last(gate_grad, gate_full) + contract_last(up_grad, up_full)
    ).astype(bf)
    tokens = partial_late.shape[0]
    n_tp = lax.axis_size(TP)
    x, c = lax.axis_index("x"), lax.axis_index("c")
    own = reduce_on_tp(partial_late, partial_early, x, c)
    outs = everywhere_on_tp(own, x, c)
    later_output = outs[:, : tokens // n_tp].reshape(tokens, -1)
    earlier_input_grad = outs[:, tokens // n_tp :].reshape(tokens, -1)

    local = local_grads(features, pieces)
    local = local.reshape(NY, rows, 3 * width)
    local = lax.all_to_all(local, "y", split_axis=0, concat_axis=0, tiled=True)
    mine = jnp.sum(local.astype(jnp.float32), axis=0).astype(bf)
    other = lax.ppermute(mine, "zh", [(0, 1), (1, 0)])
    total = mine.astype(jnp.float32) + other.astype(jnp.float32)
    return (
        later_output,
        earlier_input_grad,
        gate_sum + total[:, :width],
        up_sum + total[:, width : 2 * width],
        down_sum + total[:, 2 * width :],
    )


def solution(mesh):
    fine = Mesh(mesh.devices.reshape(2, NZL, NY, -1, 2), ("zh", "zl", "y", "x", "c"))
    tokens = P(("zh", "zl", "y"), None)
    weights = P(("zl", "y"), ("x", "c"))
    return jax.shard_map(
        per_device,
        mesh=fine,
        in_specs=(tokens,) * 3 + (weights,) * 6,
        out_specs=(tokens,) * 2 + (weights,) * 3,
        check_vma=False,
    )
```

```python
import jax
import jax.numpy as jnp
from jax import lax
from jax.sharding import Mesh, PartitionSpec as P


NZ = 8
NZL = 4
NY = 8
RING = ("zh", "zl")
TP = ("x", "c")
SHIFTS = (1, -1, -2)


def shift_z(array, by):
    return lax.ppermute(array, RING, [(i, (i + by) % NZ) for i in range(NZ)])


def contract_last(first, second):
    return lax.dot_general(
        first, second, (((1,), (1,)), ((), ())), preferred_element_type=jnp.float32
    )


def contract_first(first, second):
    return lax.dot_general(
        first, second, (((0,), (0,)), ((), ())), preferred_element_type=jnp.float32
    )


def dot(first, second):
    return jnp.dot(first, second, preferred_element_type=jnp.float32)


def shift(array, axis, count, by):
    return lax.ppermute(array, axis, [(i, (i + by) % count) for i in range(count)])


def put(buffer, block, at, dim=0):
    return lax.dynamic_update_slice_in_dim(buffer, jnp.expand_dims(block, dim), at, dim)


def spread_y(block):
    return lax.all_to_all(block, "y", split_axis=0, concat_axis=0, tiled=True)


def gather_z_then_y(shard, zl):
    near = jnp.zeros((NZL, *shard.shape), shard.dtype)
    near = put(near, shard, zl)
    for by in SHIFTS:
        block = shift_z(shard, by)
        near = put(near, block, jnp.mod(zl - by + NZL, NZL))
    full = spread_y(jnp.broadcast_to(near, (NY, *near.shape)))
    return full.transpose(1, 0, 2, 3)


def gather_y_then_z(shards, zl):
    shard = jnp.concatenate(shards, axis=1)
    column = spread_y(jnp.broadcast_to(shard, (NY, *shard.shape)))
    full = jnp.zeros((NZL, *column.shape), column.dtype)
    full = put(full, column, zl)
    for by in (1, -1):
        block = shift_z(column, by)
        full = put(full, block, jnp.mod(zl - by + NZL, NZL))
    far_low = shift_z(column[: NY // 2], 2)
    far_high = shift_z(column[NY // 2 :], -2)
    return full, far_low, far_high


def reduce_on_tp(late, early, x, c):
    n_x = lax.axis_size("x")
    tokens, width = late.shape
    cut = lambda a: a.reshape(n_x, 2, tokens // (2 * n_x), width)
    both = jnp.concatenate((cut(late), cut(early)), axis=2)
    pick = lambda at: lax.dynamic_index_in_dim(both, at, 1, keepdims=False)
    other = lax.ppermute(pick(1 - c), "c", [(0, 1), (1, 0)])
    pair = (pick(c).astype(jnp.float32) + other.astype(jnp.float32)).astype(late.dtype)
    part = lambda at: lax.dynamic_index_in_dim(pair, at, 0, keepdims=False)
    total = part(x).astype(jnp.float32)
    for by in (1, -1, 2):
        block = part(jnp.mod(x + by + n_x, n_x))
        sent = shift(block, "x", n_x, by)
        total = total + sent.astype(jnp.float32)
    return total.astype(late.dtype)


def everywhere_on_tp(own, x, c):
    n_x = lax.axis_size("x")
    line = jnp.zeros((n_x, *own.shape), own.dtype)
    line = put(line, own, x)
    for by in (1, -1, 2):
        block = shift(own, "x", n_x, by)
        line = put(line, block, jnp.mod(x - by + n_x, n_x))
    other = lax.ppermute(line, "c", [(0, 1), (1, 0)])
    both = jnp.zeros((n_x, 2, *own.shape), own.dtype)
    both = put(both, line, c, 1)
    both = put(both, other, 1 - c, 1)
    return both.reshape(2 * n_x, *own.shape)


def per_device(
    later_input,
    earlier_input,
    cotangent,
    gate_weight,
    up_weight,
    down_weight,
    gate_sum,
    up_sum,
    down_sum,
):
    bf = jnp.bfloat16
    zl = lax.axis_index("zl")
    rows, width = gate_weight.shape
    near, far_low, far_high = gather_y_then_z((up_weight, down_weight), zl)
    far = jnp.concatenate((far_low, far_high), axis=0)
    far_at = jnp.mod(zl + 2, NZL)
    part_b = put(near, far, far_at).reshape(-1, 2 * width)
    gate_full = gather_z_then_y(gate_weight, zl).reshape(-1, width)
    up_full = part_b[:, :width]
    down_full = part_b[:, width:]

    block = rows * NY

    def features_for(where):
        cut = lambda a: lax.dynamic_slice_in_dim(a, where * block, block, 1)
        return jnp.concatenate((cut(earlier_input), cut(cotangent)), axis=1)

    features = [features_for(zl)]
    for by in SHIFTS:
        sent = features_for(jnp.mod(zl + by + NZL, NZL))
        features.append(shift_z(sent, by))

    near_rows = near.reshape(-1, 2 * width)
    near_up = dot(earlier_input, near_rows[:, :width])
    near_grad = dot(cotangent, near_rows[:, width:])
    gate_early = dot(earlier_input, gate_full)
    far_x, far_cot = jnp.split(features_for(far_at), 2, axis=1)
    near_up, near_grad, far_x, far_cot = lax.optimization_barrier(
        (near_up, near_grad, far_x, far_cot)
    )
    low = far_low.reshape(-1, 2 * width)
    high = far_high.reshape(-1, 2 * width)

    n = low.shape[0]
    near_up = near_up + dot(far_x[:, :n], low[:, :width])
    near_grad = near_grad + dot(far_cot[:, :n], low[:, width:])
    near_up, near_grad = lax.optimization_barrier((near_up, near_grad))

    up_early = near_up + dot(far_x[:, n:], high[:, :width])
    hidden_grad = near_grad + dot(far_cot[:, n:], high[:, width:])
    sigmoid_gate = jax.nn.sigmoid(gate_early)
    silu_early = gate_early * sigmoid_gate
    gate_grad = (
        hidden_grad * up_early * sigmoid_gate * (1.0 + gate_early * (1.0 - sigmoid_gate))
    ).astype(bf)
    up_grad = (hidden_grad * silu_early).astype(bf)
    hidden_early = (silu_early * up_early).astype(bf)

    piece = jnp.concatenate((gate_grad, up_grad, hidden_early), axis=1)
    pieces = [piece]
    for by in SHIFTS:
        pieces.append(shift_z(piece, by))

    gate_late = dot(later_input, gate_full)
    up_late = dot(later_input, up_full)
    hidden_late = (jax.nn.silu(gate_late) * up_late).astype(bf)
    partial_late = contract_last(hidden_late, down_full).astype(bf)
    partial_early = (
        contract_last(gate_grad, gate_full) + contract_last(up_grad, up_full)
    ).astype(bf)
    tokens = partial_late.shape[0]
    n_tp = lax.axis_size(TP)
    x, c = lax.axis_index("x"), lax.axis_index("c")
    own = reduce_on_tp(partial_late, partial_early, x, c)
    outs = everywhere_on_tp(own, x, c)
    later_output = outs[:, : tokens // n_tp].reshape(tokens, -1)
    earlier_input_grad = outs[:, tokens // n_tp :].reshape(tokens, -1)

    first = jnp.concatenate(features, axis=0)
    second = jnp.concatenate(pieces, axis=0)
    both_local = contract_first(first[:, :block], second[:, : 2 * width])
    down_local = contract_first(first[:, block:], second[:, 2 * width :])
    local = jnp.concatenate((both_local.astype(bf), down_local.astype(bf)), axis=1)
    local = local.reshape(NY, rows, 3 * width)
    local = lax.all_to_all(local, "y", split_axis=0, concat_axis=0, tiled=True)
    mine = jnp.sum(local.astype(jnp.float32), axis=0).astype(bf)
    other = lax.ppermute(mine, "zh", [(0, 1), (1, 0)])
    total = mine.astype(jnp.float32) + other.astype(jnp.float32)
    return (
        later_output,
        earlier_input_grad,
        gate_sum + total[:, :width],
        up_sum + total[:, width : 2 * width],
        down_sum + total[:, 2 * width :],
    )


def solution(mesh):
    fine = Mesh(mesh.devices.reshape(2, NZL, NY, -1, 2), ("zh", "zl", "y", "x", "c"))
    tokens = P(("zh", "zl", "y"), None)
    weights = P(("zl", "y"), ("x", "c"))
    return jax.shard_map(
        per_device,
        mesh=fine,
        in_specs=(tokens,) * 3 + (weights,) * 6,
        out_specs=(tokens,) * 2 + (weights,) * 3,
        check_vma=False,
    )
```
